32 devices in a mesh: sp: 16 (over z, y, x), tp: 2 (over core).
Axes of the slice: x: 2, y: 2, z: 4, core: 2. Of those that a mesh axis runs over, the one named last changes fastest.
Arguments:
- residual: bfloat16 [4096, 2048], P(('sp', 'tp')), may hold values from -6 to 6
- query_nope: bfloat16 [4096, 1024], P('sp', 'tp'), may hold values from -24 to 24
- query_rope: bfloat16 [4096, 512], P('sp', 'tp'), may hold values from -400 to 400
- latent: bfloat16 [4096, 256], P(('sp', 'tp')), may hold values from -6 to 6
- key_rope: bfloat16 [4096, 64], P(('sp', 'tp')), may hold values from -6 to 6
- key_up: bfloat16 [256, 1024], P(None, 'tp'), may hold values from -0.375 to 0.375
- value_up: bfloat16 [256, 1024], P(None, 'tp'), may hold values from -0.375 to 0.375
- out_proj: bfloat16 [1024, 2048], replicated, may hold values from -0.375 to 0.375
- norm_gain: float32 [2048], replicated, may hold values from 0.1 to 1.9
- routes: int32 [4096, 2], P(('sp', 'tp')), may hold values from 0 to 15, all different within a row; in each aligned block of 128 rows (0 to 127, 128 to 255, ...) at most 32 rows name the same one
- route_weight: float32 [4096, 2], P(('sp', 'tp')), may hold values from 0.3 to 2.5
- w_gate: bfloat16 [16, 2048, 512], P('sp', None, 'tp'), may hold values from -0.125 to 0.125
- w_up: bfloat16 [16, 2048, 512], P('sp', None, 'tp'), may hold values from -0.125 to 0.125
- w_down: bfloat16 [16, 512, 2048], P('sp', 'tp'), may hold values from -0.25 to 0.25
Outputs:
- mixed: bfloat16 [4096, 2048], P(('sp', 'tp'))
The draws below stay inside these ranges and needn't reach their ends.
Inputs may be any that keep to these rules, and one draw needn't show every extreme that they name: `routes`: each row names 2 different experts. Among the rows of one device no expert is named more than 32 times, a bound that some block reaches by the rows of some device.
All inputs are finite; a program needn't handle non-finite values.
Results may differ from the reference program's by a relative error of at most 0.015.
Values may be sent and summed in bfloat16 or wider, within the bound.
A program may use at most 128 MiB of HBM per device.

```python
import math
import jax
import jax.numpy as jnp
import numpy as np
from jax import lax

D = 2048
HEADS = 8
QK_NOPE = 128
QK_ROPE = 64
V_DIM = 128
LATENT = 256
FF = 512
TOP = 2
SEGMENT = 64
TOK_DEV = 256
TOKENS = 4096
EXPERTS = 16
CAP = 32
N_SP = 16
N_TP = 2


def draw_key_rope(key, part):
    noise = jax.random.truncated_normal(jax.random.fold_in(key, 31), -6.0, 6.0, (TOKENS, QK_ROPE), jnp.float32)
    return noise.astype(jnp.bfloat16)


def draw_query_rope(key, part):
    noise = jax.random.truncated_normal(jax.random.fold_in(key, 32), -6.0, 6.0, (TOKENS, HEADS * QK_ROPE), jnp.float32)
    return noise.astype(jnp.bfloat16)


def steps_of(rng, dims, shards, low, largest):
    loudness, own = 1.0, jax.random.fold_in(rng, 6)
    for dim, blocks in shards:
        heights = jnp.exp(jax.random.uniform(jax.random.fold_in(own, dim), (blocks,), jnp.float32, low / len(shards), largest / len(shards)))
        loudness = loudness * jnp.repeat(heights, dims[dim] // blocks).reshape([-1 if axis == dim else 1 for axis in range(len(dims))])
    return loudness


def routed_block(key, own, number, rows, number_of, top, reach, skew):
    order = jax.random.permutation(key, number_of)
    crowded, usual = load_shares(number_of, rows * top, reach, skew, True), load_shares(number_of, rows * top, reach, skew, False)
    places = jnp.arange(number_of)

    def named(sizes, turn):
        used = int((sizes > 0).sum())
        fixed = max(1, used // 4)
        moved = fixed + (places - fixed + turn * (used - fixed)) % max(1, number_of - fixed)
        return jnp.zeros((number_of,), jnp.int32).at[order[jnp.where(places < fixed, places, moved)]].set(jnp.asarray(sizes, jnp.int32))

    sizes = jnp.where(number % 4 == 0, named(crowded, number // 4), named(usual, number - number // 4 - 1))
    mixed = jax.random.permutation(jax.random.fold_in(own, 3), number_of)
    donor, taker = mixed[0:number_of // 2 * 2:2], mixed[1:number_of // 2 * 2:2]
    slack = jnp.minimum(sizes[donor] - 1, reach - sizes[taker]) // 2
    slack = jnp.where((donor == order[0]) | (taker == order[0]) | (sizes[taker] == 0), 0, jnp.maximum(slack, 0))
    moved = jax.random.randint(jax.random.fold_in(own, 4), (number_of // 2,), 0, 1 << 20) % (slack + 1)
    sizes = sizes.at[donor].add(-moved).at[taker].add(moved)
    items = jnp.searchsorted(jnp.cumsum(sizes), jnp.arange(rows * top), side="right").astype(jnp.int32)
    grid = items.reshape(top, rows).T
    grid = grid[jax.random.permutation(jax.random.fold_in(own, 1), rows)]
    turn = jax.random.randint(jax.random.fold_in(own, 2), (rows, 1), 0, top)
    return jnp.take_along_axis(grid, (jnp.arange(top)[None, :] + turn) % top, axis=1)


def load_shares(count, total, most, slope, full):
    weights = [(1 << 20) // math.isqrt(standing ** slope) + 1 for standing in range(1, count + 1)]
    largest = most if full else min(most, max(-(-total // count), total * weights[0] // sum(weights)))
    least = 1 if total - largest >= count - 1 else 0
    holding, surplus = [largest] + [least] * (count - 1), total - largest - least * (count - 1)
    while surplus > 0:
        movable = [i for i in range(1, count) if holding[i] < largest] or [i for i in range(1, count) if holding[i] < most]
        whole, budget = sum([weights[i] for i in movable]), surplus
        for i in movable:
            addition = min(most - holding[i], max(1, budget * weights[i] // whole), surplus)
            holding[i] = holding[i] + addition
            surplus = surplus - addition
    return np.array(holding)


def normal_values(own_key, shape, width, most, split=(), held_as=jnp.bfloat16):
    values = jax.random.normal(own_key, shape, jnp.float32) * width
    if len(split) > 0:
        values = steps_of(own_key, shape, split, -0.22, 0.18) * values
    return jnp.clip(values, min=-most, max=most).astype(held_as)


def setup_inputs(seed: int = 0) -> dict:
    keys = jax.random.split(jax.random.key(seed), 15)
    residual = normal_values(keys[0], (TOKENS, D), 1.0, 6.0, ((0, 32),))
    query_nope = normal_values(keys[1], (TOKENS, HEADS * QK_NOPE), 4.0, 24.0, ((0, 16), (1, 2)))
    query_rope = draw_query_rope(jax.random.fold_in(keys[14], 71), 0)
    latent = normal_values(keys[3], (TOKENS, LATENT), 1.0, 6.0, ((0, 32),))
    key_rope = draw_key_rope(jax.random.fold_in(keys[14], 71), 0)
    key_up = normal_values(keys[5], (LATENT, HEADS * QK_NOPE), LATENT ** -0.5, 0.375, ((1, 2),))
    value_up = normal_values(keys[6], (LATENT, HEADS * V_DIM), LATENT ** -0.5, 0.375, ((1, 2),))
    out_proj = normal_values(keys[7], (HEADS * V_DIM, D), (HEADS * V_DIM // 4) ** -0.5, 0.375)
    norm_gain = jnp.clip(1.0 + 0.18 * jax.random.normal(keys[8], (D,), jnp.float32), 0.1, 1.9)
    routes_keys = jax.random.split(jax.random.fold_in(keys[9], 1), TOKENS // (TOK_DEV // N_TP))
    routes_turns = jax.random.permutation(jax.random.fold_in(keys[9], 3), TOKENS // (TOK_DEV // N_TP))
    routes = jax.vmap(lambda own, number: routed_block(jax.random.fold_in(keys[9], 2), own, number, TOK_DEV // N_TP, EXPERTS, TOP, CAP, 2))(routes_keys, routes_turns).reshape((TOKENS, TOP))
    route_weight = jnp.clip(jnp.exp(math.log(2.5) - 2.1202635 * jax.random.uniform(keys[10], (TOKENS, TOP), jnp.float32) ** steps_of(keys[10], (TOKENS, TOP), ((0, 32),), -0.2, 0.2)), 0.3, 2.5)
    w_gate = normal_values(keys[11], (EXPERTS, D, FF), D ** -0.5, 0.125, ((0, 16), (2, 2)))
    w_up = normal_values(keys[12], (EXPERTS, D, FF), D ** -0.5, 0.125, ((0, 16), (2, 2)))
    w_down = normal_values(keys[13], (EXPERTS, FF, D), FF ** -0.5, 0.25, ((0, 16), (1, 2)))
    return dict(residual=residual, query_nope=query_nope, query_rope=query_rope, latent=latent, key_rope=key_rope, key_up=key_up, value_up=value_up, out_proj=out_proj, norm_gain=norm_gain, routes=routes, route_weight=route_weight, w_gate=w_gate, w_up=w_up, w_down=w_down)


EPSILON = 1e-06
ROPE_BASE = 10000.0

def rotary(values, positions):
    half_width = values.shape[-1] // 2
    inverse = ROPE_BASE ** (-2.0 * jnp.arange(half_width, dtype=jnp.float32) / values.shape[-1])
    angles = positions.astype(jnp.float32)[:, None] * inverse[None, :]
    cosine = jnp.cos(angles)
    sine_part = jnp.sin(angles)
    if values.ndim == 3:
        cosine = cosine[:, None, :]
        sine_part = sine_part[:, None, :]
    first_half = values[..., :half_width]
    second = values[..., half_width:]
    return jnp.concatenate([first_half * cosine - second * sine_part, second * cosine + first_half * sine_part], axis=-1)

def reference(residual, query_nope, query_rope, latent, key_rope, key_up, value_up, out_proj, norm_gain, routes, route_weight, w_gate, w_up, w_down):
    positions = jnp.arange(TOKENS, dtype=jnp.int32)
    query_rot = rotary(query_rope.astype(jnp.float32).reshape(TOKENS, HEADS, QK_ROPE), positions).astype(jnp.bfloat16)
    key_rot = rotary(key_rope.astype(jnp.float32), positions).astype(jnp.bfloat16)
    key_nope = jnp.dot(latent, key_up, preferred_element_type=jnp.float32).astype(jnp.bfloat16)
    value_rows = jnp.dot(latent, value_up, preferred_element_type=jnp.float32).astype(jnp.bfloat16)
    keys_wide = key_nope.astype(jnp.float32).reshape(TOKENS, HEADS, QK_NOPE)
    values_wide = value_rows.astype(jnp.float32).reshape(TOKENS, HEADS, V_DIM)
    rot_wide = key_rot.astype(jnp.float32)
    query_wide = query_nope.astype(jnp.float32).reshape(TOKENS, HEADS, QK_NOPE)
    query_rot_wide = query_rot.astype(jnp.float32)
    score_scale = (QK_NOPE + QK_ROPE) ** (-0.5)
    key_segment = positions // SEGMENT
    query_block = math.gcd(TOKENS, 512)

    def one_block(block_index):
        first_row = (block_index * query_block).astype(jnp.int32)
        query_part = lax.dynamic_slice_in_dim(query_wide, first_row, query_block, 0)
        rot_part = lax.dynamic_slice_in_dim(query_rot_wide, first_row, query_block, 0)
        scores = jnp.einsum('qhd,khd->hqk', query_part, keys_wide)
        scores = (scores + jnp.einsum('qhr,kr->hqk', rot_part, rot_wide)) * score_scale
        query_segment = (first_row + jnp.arange(query_block, dtype=jnp.int32)) // SEGMENT
        allowed = (key_segment[None, :] <= query_segment[:, None])[None]
        scores = jnp.where(allowed, scores, -jnp.inf)
        row_max = lax.optimization_barrier(jnp.max(scores, axis=-1, keepdims=True))
        weights = jnp.exp(scores - row_max)
        weight_sum = lax.optimization_barrier(jnp.sum(weights, axis=-1))
        weights_low = lax.optimization_barrier(weights.astype(jnp.bfloat16)).astype(jnp.float32)
        weighted = jnp.einsum('hqk,khv->qhv', weights_low, values_wide)
        return weighted / weight_sum.T[:, :, None]
    attn_out = lax.map(one_block, jnp.arange(TOKENS // query_block, dtype=jnp.int32))
    attn_out = attn_out.reshape(TOKENS, HEADS * V_DIM).astype(jnp.bfloat16)
    projected = jnp.dot(attn_out, out_proj, preferred_element_type=jnp.float32)
    hidden = (residual.astype(jnp.float32) + projected).astype(jnp.bfloat16)
    hidden_wide = hidden.astype(jnp.float32)
    normed = hidden_wide * lax.rsqrt(lax.optimization_barrier(jnp.mean(hidden_wide * hidden_wide, axis=-1, keepdims=True)) + EPSILON)
    normed = (normed * norm_gain[None, :]).astype(jnp.bfloat16)
    buffer_rows = N_TP * N_SP * CAP
    flat_expert = routes.reshape(-1).astype(jnp.int32)
    onehot = (flat_expert[:, None] == jnp.arange(EXPERTS, dtype=jnp.int32)[None, :]).astype(jnp.int32)
    slot_rank = lax.optimization_barrier(jnp.sum(jnp.cumsum(onehot, axis=0) * onehot, axis=1)) - 1
    slot_index = (flat_expert * buffer_rows + slot_rank).astype(jnp.int32)
    buffer = jnp.zeros((EXPERTS * buffer_rows, D), jnp.bfloat16).at[slot_index].set(jnp.repeat(normed, TOP, axis=0))

    def expert_rows(inputs):
        rows_in, gate_weight, up_weight, down_weight = inputs
        gate_part = jnp.dot(rows_in, gate_weight, preferred_element_type=jnp.float32)
        up_part = jnp.dot(rows_in, up_weight, preferred_element_type=jnp.float32)
        activated = lax.optimization_barrier((jax.nn.silu(gate_part) * up_part).astype(jnp.bfloat16))
        parts = jnp.einsum('bpf,pfd->pbd', activated.astype(jnp.float32).reshape(buffer_rows, N_TP, FF // N_TP), down_weight.astype(jnp.float32).reshape(N_TP, FF // N_TP, D))
        half_out = lax.optimization_barrier(parts.astype(jnp.bfloat16)).astype(jnp.float32)
        return lax.optimization_barrier(jnp.sum(half_out, axis=0)).astype(jnp.bfloat16)
    outputs = lax.map(expert_rows, (buffer.reshape(EXPERTS, buffer_rows, D), w_gate, w_up, w_down))
    picked = outputs.reshape(EXPERTS * buffer_rows, D)[slot_index]
    combined = lax.optimization_barrier(jnp.sum(picked.astype(jnp.float32).reshape(TOKENS, TOP, D) * route_weight[:, :, None], axis=1))
    return (hidden_wide + combined).astype(jnp.bfloat16)
```

```python
import functools
import math

import jax
import jax.numpy as jnp
from jax import lax
from jax.experimental import pallas as pl
from jax.experimental.pallas import tpu as pltpu
from jax.sharding import PartitionSpec as P

QK_NOPE = 128
QK_ROPE = 64
V_DIM = 128
SEGMENT = 64


EPSILON = 1e-06
ROPE_BASE = 10000.0
NEG_LARGE = -1e30


def rotary(values, positions):
    half_width = values.shape[-1] // 2
    inverse = ROPE_BASE ** (-2.0 * jnp.arange(half_width, dtype=jnp.float32) / values.shape[-1])
    angles = positions.astype(jnp.float32)[:, None] * inverse[None, :]
    cosine = jnp.cos(angles)
    sine_part = jnp.sin(angles)
    if values.ndim == 3:
        cosine = cosine[:, None, :]
        sine_part = sine_part[:, None, :]
    first_half = values[..., :half_width]
    second = values[..., half_width:]
    return jnp.concatenate(
        [first_half * cosine - second * sine_part, second * cosine + first_half * sine_part],
        axis=-1,
    )


MESH = pl.DeviceIdType.MESH
VMEM = pl.BlockSpec(memory_space=pltpu.VMEM)


def greet(peers):
    barrier = pltpu.get_barrier_semaphore()
    for peer in peers:
        pl.semaphore_signal(barrier, inc=1, device_id=peer, device_id_type=MESH)
    pl.semaphore_wait(barrier, len(peers))


def far_first(count):
    return sorted(range(1, count), key=lambda step: abs(2 * step - count))


def send(source, target, send_sem, recv_sem, peer):
    copy = pltpu.make_async_remote_copy(
        src_ref=source,
        dst_ref=target,
        send_sem=send_sem,
        recv_sem=recv_sem,
        device_id=peer,
        device_id_type=MESH,
    )
    copy.start()
    return copy


def arrived(block, semaphore):
    pltpu.make_async_copy(block, block, semaphore).wait()


def gather_kernel(n_sp, n_tp, inner, own_ref, out_ref, send_sem, recv_sem, local_sem):
    sp, tp = lax.axis_index("sp"), lax.axis_index("tp")
    outer = n_sp // inner
    group, member = sp // inner, sp % inner

    def column(step):
        return ((group + step) % outer) * inner + member

    def mate(step):
        return group * inner + (member + step) % inner

    others = [(column(step), tp) for step in far_first(outer)]
    mates = [(mate(step), tp) for step in range(1, inner)]
    twins = [(sp, (tp + step) % n_tp) for step in range(1, n_tp)]
    greet(others + mates + twins)
    copies = []

    def push(source, block, peers):
        for peer in peers:
            copies.append(
                send(
                    source, out_ref.at[block], send_sem.at[len(copies)], recv_sem.at[block], peer
                )
            )

    mine = sp * n_tp + tp
    keep = pltpu.make_async_copy(own_ref, out_ref.at[mine], local_sem)
    keep.start()
    push(own_ref, mine, others + mates + twins)
    for step in sorted(range(1, outer), key=lambda step: min(step, outer - step)):
        block = column(step) * n_tp + tp
        arrived(out_ref.at[block], recv_sem.at[block])
        push(out_ref.at[block], block, mates + twins)
    for step in range(outer):
        for hop in range(1, inner):
            source = ((group + step) % outer) * inner + (member + hop) % inner
            block = source * n_tp + tp
            arrived(out_ref.at[block], recv_sem.at[block])
            push(out_ref.at[block], block, twins)
    for twin in twins:
        for source in range(n_sp):
            block = source * n_tp + twin[1]
            arrived(out_ref.at[block], recv_sem.at[block])
    keep.wait()
    for copy in copies:
        copy.wait_send()


def gather_rows(own, n_sp, n_tp):
    inner = math.gcd(n_sp, 4)
    outer = n_sp // inner
    sends = (outer - 1) + outer * (inner - 1) + n_sp * (n_tp - 1)
    return pl.pallas_call(
        functools.partial(gather_kernel, n_sp, n_tp, inner),
        out_shape=jax.ShapeDtypeStruct((n_sp * n_tp,) + own.shape, own.dtype),
        in_specs=[VMEM],
        out_specs=VMEM,
        scratch_shapes=[
            pltpu.SemaphoreType.DMA((sends,)),
            pltpu.SemaphoreType.DMA((n_sp * n_tp,)),
            pltpu.SemaphoreType.DMA,
        ],
        compiler_params=pltpu.CompilerParams(collective_id=0, has_side_effects=True),
        name="gather_rows",
    )(own)


def dispatch_kernel(n_sp, n_tp, rows_ref, out_ref, send_sem, recv_sem, local_sem):
    sp, tp = lax.axis_index("sp"), lax.axis_index("tp")
    peers = [((sp + step) % n_sp, tp) for step in far_first(n_sp)]
    twins = [(sp, (tp + step) % n_tp) for step in range(1, n_tp)]
    greet(peers + twins)
    copies = []

    def push(source, core, origin, peer):
        copies.append(
            send(
                source,
                out_ref.at[core, origin],
                send_sem.at[len(copies)],
                recv_sem.at[core * n_sp + origin],
                peer,
            )
        )

    keep = pltpu.make_async_copy(rows_ref.at[sp], out_ref.at[tp, sp], local_sem)
    keep.start()
    for peer in peers:
        push(rows_ref.at[peer[0]], tp, sp, peer)
    for twin in twins:
        push(rows_ref.at[sp], tp, sp, twin)
    for step in reversed(far_first(n_sp)):
        origin = (sp + step) % n_sp
        arrived(out_ref.at[tp, origin], recv_sem.at[tp * n_sp + origin])
        for twin in twins:
            push(out_ref.at[tp, origin], tp, origin, twin)
    for twin in twins:
        for origin in range(n_sp):
            arrived(out_ref.at[twin[1], origin], recv_sem.at[twin[1] * n_sp + origin])
    keep.wait()
    for copy in copies:
        copy.wait_send()


def dispatch_rows(rows, n_sp, n_tp):
    sends = n_sp - 1 + n_sp * (n_tp - 1)
    return pl.pallas_call(
        functools.partial(dispatch_kernel, n_sp, n_tp),
        out_shape=jax.ShapeDtypeStruct((n_tp,) + rows.shape, rows.dtype),
        in_specs=[VMEM],
        out_specs=VMEM,
        scratch_shapes=[
            pltpu.SemaphoreType.DMA((sends,)),
            pltpu.SemaphoreType.DMA((n_sp * n_tp,)),
            pltpu.SemaphoreType.DMA,
        ],
        compiler_params=pltpu.CompilerParams(collective_id=1, has_side_effects=True),
        name="dispatch_rows",
    )(rows)


def return_kernel(
    n_sp, n_tp, part_ref, out_ref, half_ref, sum_ref, twin_send, twin_recv, send_sem, recv_sem, local_sem
):
    sp, tp = lax.axis_index("sp"), lax.axis_index("tp")
    order = far_first(n_sp)
    peers = [((sp + step) % n_sp, tp) for step in order]
    twins = [(sp, (tp + step) % n_tp) for step in range(1, n_tp)]
    greet(peers + twins)
    copies = []
    for target in [peer[0] for peer in peers] + [sp]:
        for step, twin in enumerate(twins):
            slot = step * n_sp + target
            copies.append(
                send(
                    part_ref.at[twin[1], target],
                    half_ref.at[step, target],
                    twin_send.at[slot],
                    twin_recv.at[slot],
                    twin,
                )
            )

    def total(target):
        value = part_ref[tp, target].astype(jnp.float32)
        for step in range(n_tp - 1):
            arrived(half_ref.at[step, target], twin_recv.at[step * n_sp + target])
            value = value + half_ref[step, target].astype(jnp.float32)
        sum_ref[target] = value.astype(sum_ref.dtype)

    for number, peer in enumerate(peers):
        total(peer[0])
        copies.append(
            send(sum_ref.at[peer[0]], out_ref.at[sp], send_sem.at[number], recv_sem.at[sp], peer)
        )
    total(sp)
    keep = pltpu.make_async_copy(sum_ref.at[sp], out_ref.at[sp], local_sem)
    keep.start()
    for step in reversed(order):
        origin = (sp + step) % n_sp
        arrived(out_ref.at[origin], recv_sem.at[origin])
    keep.wait()
    for copy in copies:
        copy.wait_send()


def return_rows(parts, n_sp, n_tp):
    shape = parts.shape[1:]
    return pl.pallas_call(
        functools.partial(return_kernel, n_sp, n_tp),
        out_shape=jax.ShapeDtypeStruct(shape, parts.dtype),
        in_specs=[VMEM],
        out_specs=VMEM,
        scratch_shapes=[
            pltpu.VMEM((n_tp - 1,) + shape, parts.dtype),
            pltpu.VMEM(shape, parts.dtype),
            pltpu.SemaphoreType.DMA(((n_tp - 1) * n_sp,)),
            pltpu.SemaphoreType.DMA(((n_tp - 1) * n_sp,)),
            pltpu.SemaphoreType.DMA((n_sp - 1,)),
            pltpu.SemaphoreType.DMA((n_sp,)),
            pltpu.SemaphoreType.DMA,
        ],
        compiler_params=pltpu.CompilerParams(collective_id=2, has_side_effects=True),
        name="return_rows",
    )(parts)


NT = (((1,), (1,)), ((), ()))


def attention_kernel(
    key_block, latent_width, heads, base_ref, query_ref, kv_ref, key_up_ref, value_up_ref, out_ref, max_ref, sum_ref, acc_ref
):
    first = base_ref[0]
    queries = query_ref.shape[2]
    scale = (QK_NOPE + QK_ROPE) ** (-0.5) * math.log2(math.e)
    max_ref[...] = jnp.full_like(max_ref, NEG_LARGE)
    sum_ref[...] = jnp.zeros_like(sum_ref)
    acc_ref[...] = jnp.zeros_like(acc_ref)

    def block(start, masked):
        start = pl.multiple_of(start, key_block)
        rows = kv_ref[pl.ds(start, key_block), :]
        latent = rows[:, :latent_width]
        rot = rows[:, latent_width:]
        keys = jnp.dot(latent, key_up_ref[...], preferred_element_type=jnp.float32).astype(
            jnp.bfloat16
        )
        values = lax.dot_general(
            value_up_ref[...], latent, NT, preferred_element_type=jnp.float32
        ).astype(jnp.bfloat16)
        if masked:
            key_segment = (
                start + lax.broadcasted_iota(jnp.int32, (key_block, queries), 0)
            ) // SEGMENT
            query_segment = (
                first + lax.broadcasted_iota(jnp.int32, (key_block, queries), 1)
            ) // SEGMENT
            allowed = key_segment <= query_segment
        for head in range(heads):
            wide = jnp.concatenate([keys[:, head * QK_NOPE : (head + 1) * QK_NOPE], rot], axis=1)
            scores = jnp.dot(wide, query_ref[head], preferred_element_type=jnp.float32)
            if masked:
                scores = jnp.where(allowed, scores, NEG_LARGE)
            old_max = max_ref[head]
            new_max = jnp.maximum(old_max, jnp.max(scores, axis=0, keepdims=True))
            weights = jnp.exp2((scores - new_max) * scale)
            shrink = jnp.exp2((old_max - new_max) * scale)
            max_ref[head] = new_max
            sum_ref[head] = sum_ref[head] * shrink + jnp.sum(weights, axis=0, keepdims=True)
            acc_ref[head] = acc_ref[head] * shrink + jnp.dot(
                values[head * V_DIM : (head + 1) * V_DIM],
                weights.astype(jnp.bfloat16),
                preferred_element_type=jnp.float32,
            )

    whole = first // key_block

    def body(step, carry):
        block(step * key_block, False)
        return carry

    lax.fori_loop(0, whole, body, 0)
    block(whole * key_block, True)
    for head in range(heads):
        out_ref[:, head * V_DIM : (head + 1) * V_DIM] = (
            (acc_ref[head] / sum_ref[head]).T.astype(out_ref.dtype)
        )


def attention(base, query, kv, key_up, value_up_t, key_block, latent_width):
    heads, unused, queries = query.shape
    return pl.pallas_call(
        functools.partial(attention_kernel, key_block, latent_width, heads),
        out_shape=jax.ShapeDtypeStruct((queries, heads * V_DIM), jnp.bfloat16),
        in_specs=[pl.BlockSpec(memory_space=pltpu.SMEM), VMEM, VMEM, VMEM, VMEM],
        out_specs=VMEM,
        scratch_shapes=[
            pltpu.VMEM((heads, 1, queries), jnp.float32),
            pltpu.VMEM((heads, 1, queries), jnp.float32),
            pltpu.VMEM((heads, V_DIM, queries), jnp.float32),
        ],
        name="attention",
    )(base, query, kv, key_up, value_up_t)


def local(
    residual,
    query_nope,
    query_rope,
    latent,
    key_rope,
    key_up,
    value_up,
    out_proj,
    norm_gain,
    routes,
    route_weight,
    w_gate,
    w_up,
    w_down,
):
    tp_count = lax.axis_size("tp")
    sp_count = lax.axis_size("sp")
    tp_index = lax.axis_index("tp")
    sp_index = lax.axis_index("sp")
    row_count = residual.shape[0]
    tok_dev = query_nope.shape[0]
    heads_here = query_nope.shape[1] // QK_NOPE
    query_first = sp_index * tok_dev
    query_pos = query_first + jnp.arange(tok_dev, dtype=jnp.int32)
    query_rot = rotary(
        query_rope.astype(jnp.float32).reshape(tok_dev, heads_here, QK_ROPE), query_pos
    ).astype(jnp.bfloat16)
    query_heads = query_nope.reshape(tok_dev, heads_here, QK_NOPE)
    key_pos = query_first + tp_index * row_count + jnp.arange(row_count, dtype=jnp.int32)
    key_rot = rotary(key_rope.astype(jnp.float32), key_pos).astype(jnp.bfloat16)
    width_pad = -(-QK_ROPE // 128) * 128 - QK_ROPE
    packed = jnp.concatenate(
        [latent, key_rot, jnp.zeros((row_count, width_pad), jnp.bfloat16)], axis=1
    )
    gathered = gather_rows(packed, sp_count, tp_count)
    kv_rows = gathered.reshape(sp_count * tok_dev, packed.shape[1])
    query = jnp.concatenate(
        [query_heads, query_rot, jnp.zeros((tok_dev, heads_here, width_pad), jnp.bfloat16)], axis=2
    ).transpose(1, 2, 0)
    key_block = tok_dev * math.gcd(sp_count, 2)
    attn_out = attention(
        query_first.astype(jnp.int32).reshape(1),
        query,
        kv_rows,
        key_up,
        value_up.T,
        key_block,
        latent.shape[1],
    )
    all_heads = lax.all_to_all(attn_out, "tp", split_axis=0, concat_axis=1, tiled=True)
    projected = jnp.dot(all_heads, out_proj, preferred_element_type=jnp.float32)
    hidden_wide = residual.astype(jnp.float32) + projected
    hidden = hidden_wide.astype(jnp.bfloat16)
    hidden_wide = hidden.astype(jnp.float32)
    normed = hidden_wide * lax.rsqrt(
        jnp.mean(hidden_wide * hidden_wide, axis=-1, keepdims=True) + EPSILON
    )
    normed = (normed * norm_gain[None, :]).astype(jnp.bfloat16)
    expert_count = lax.axis_size("sp")
    capacity = max(2, 2 * (row_count * tp_count) // expert_count)
    top_count = routes.shape[1]
    width = normed.shape[1]
    flat_expert = routes.reshape(-1)
    onehot = (flat_expert[:, None] == jnp.arange(expert_count, dtype=jnp.int32)[None, :]).astype(
        jnp.int32
    )
    slot_rank = jnp.sum(jnp.cumsum(onehot, axis=0) * onehot, axis=1) - 1
    slot_index = flat_expert * capacity + slot_rank
    slots = slot_index.reshape(row_count, top_count)
    slot_count = expert_count * capacity
    numbers = jnp.arange(slot_count, dtype=jnp.int32)
    chosen = slots[:, :, None] == numbers[None, None, :]
    place = jnp.any(chosen, axis=1).astype(jnp.bfloat16)
    outgoing = lax.dot_general(
        place, normed, (((0,), (0,)), ((), ())), preferred_element_type=jnp.float32
    ).astype(jnp.bfloat16)
    shares = jnp.sum(jnp.where(chosen, route_weight[:, :, None], 0.0), axis=1)
    share_high = lax.reduce_precision(shares, 8, 7)
    share_low = shares - share_high
    received = dispatch_rows(
        outgoing.reshape(expert_count, capacity, width), sp_count, tp_count
    ).reshape(tp_count * slot_count, width)
    gate_part = jnp.dot(received, w_gate[0], preferred_element_type=jnp.float32)
    up_part = jnp.dot(received, w_up[0], preferred_element_type=jnp.float32)
    activated = (jax.nn.silu(gate_part) * up_part).astype(jnp.bfloat16)
    product = jnp.dot(activated, w_down[0], preferred_element_type=jnp.float32).astype(jnp.bfloat16)
    back_rows = return_rows(
        product.reshape(tp_count, expert_count, capacity, width), sp_count, tp_count
    ).reshape(slot_count, width)
    combined = jnp.dot(
        share_high.astype(jnp.bfloat16), back_rows, preferred_element_type=jnp.float32
    ) + jnp.dot(share_low.astype(jnp.bfloat16), back_rows, preferred_element_type=jnp.float32)
    return (hidden_wide + combined).astype(jnp.bfloat16)


def solution(mesh):
    return jax.shard_map(
        local,
        mesh=mesh,
        in_specs=(
            P(("sp", "tp"), None),
            P("sp", "tp"),
            P("sp", "tp"),
            P(("sp", "tp"), None),
            P(("sp", "tp"), None),
            P(None, "tp"),
            P(None, "tp"),
            P(),
            P(),
            P(("sp", "tp"), None),
            P(("sp", "tp"), None),
            P("sp", None, "tp"),
            P("sp", None, "tp"),
            P("sp", "tp", None),
        ),
        out_specs=P(("sp", "tp"), None),
        check_vma=False,
    )
```

```python
import functools
import math

import jax
import jax.numpy as jnp
from jax import lax
from jax.experimental import pallas as pl
from jax.experimental.pallas import tpu as pltpu
from jax.sharding import PartitionSpec as P

QK_NOPE = 128
QK_ROPE = 64
V_DIM = 128
SEGMENT = 64


EPSILON = 1e-06
ROPE_BASE = 10000.0
NEG_LARGE = -1e30


def rotary(values, positions):
    half_width = values.shape[-1] // 2
    inverse = ROPE_BASE ** (-2.0 * jnp.arange(half_width, dtype=jnp.float32) / values.shape[-1])
    angles = positions.astype(jnp.float32)[:, None] * inverse[None, :]
    cosine = jnp.cos(angles)
    sine_part = jnp.sin(angles)
    if values.ndim == 3:
        cosine = cosine[:, None, :]
        sine_part = sine_part[:, None, :]
    first_half = values[..., :half_width]
    second = values[..., half_width:]
    return jnp.concatenate(
        [first_half * cosine - second * sine_part, second * cosine + first_half * sine_part],
        axis=-1,
    )


MESH = pl.DeviceIdType.MESH
VMEM = pl.BlockSpec(memory_space=pltpu.VMEM)


def greet(peers):
    barrier = pltpu.get_barrier_semaphore()
    for peer in peers:
        pl.semaphore_signal(barrier, inc=1, device_id=peer, device_id_type=MESH)
    pl.semaphore_wait(barrier, len(peers))


def far_first(count):
    return sorted(range(1, count), key=lambda step: abs(2 * step - count))


def send(source, target, send_sem, recv_sem, peer):
    copy = pltpu.make_async_remote_copy(
        src_ref=source,
        dst_ref=target,
        send_sem=send_sem,
        recv_sem=recv_sem,
        device_id=peer,
        device_id_type=MESH,
    )
    copy.start()
    return copy


def arrived(block, semaphore):
    pltpu.make_async_copy(block, block, semaphore).wait()


def gather_kernel(n_sp, n_tp, inner, own_ref, out_ref, send_sem, recv_sem, local_sem):
    sp, tp = lax.axis_index("sp"), lax.axis_index("tp")
    outer = n_sp // inner
    group, member = sp // inner, sp % inner

    def column(step):
        return ((group + step) % outer) * inner + member

    def mate(step):
        return group * inner + (member + step) % inner

    others = [(column(step), tp) for step in far_first(outer)]
    mates = [(mate(step), tp) for step in range(1, inner)]
    twins = [(sp, (tp + step) % n_tp) for step in range(1, n_tp)]
    greet(others + mates + twins)
    copies = []

    def push(source, block, peers):
        for peer in peers:
            copies.append(
                send(
                    source, out_ref.at[block], send_sem.at[len(copies)], recv_sem.at[block], peer
                )
            )

    mine = sp * n_tp + tp
    keep = pltpu.make_async_copy(own_ref, out_ref.at[mine], local_sem)
    keep.start()
    push(own_ref, mine, others + mates + twins)
    for step in sorted(range(1, outer), key=lambda step: min(step, outer - step)):
        block = column(step) * n_tp + tp
        arrived(out_ref.at[block], recv_sem.at[block])
        push(out_ref.at[block], block, mates + twins)
    for step in range(outer):
        for hop in range(1, inner):
            source = ((group + step) % outer) * inner + (member + hop) % inner
            block = source * n_tp + tp
            arrived(out_ref.at[block], recv_sem.at[block])
            push(out_ref.at[block], block, twins)
    for twin in twins:
        for source in range(n_sp):
            block = source * n_tp + twin[1]
            arrived(out_ref.at[block], recv_sem.at[block])
    keep.wait()
    for copy in copies:
        copy.wait_send()


def gather_rows(own, n_sp, n_tp):
    inner = math.gcd(n_sp, 4)
    outer = n_sp // inner
    sends = (outer - 1) + outer * (inner - 1) + n_sp * (n_tp - 1)
    return pl.pallas_call(
        functools.partial(gather_kernel, n_sp, n_tp, inner),
        out_shape=jax.ShapeDtypeStruct((n_sp * n_tp,) + own.shape, own.dtype),
        in_specs=[VMEM],
        out_specs=VMEM,
        scratch_shapes=[
            pltpu.SemaphoreType.DMA((sends,)),
            pltpu.SemaphoreType.DMA((n_sp * n_tp,)),
            pltpu.SemaphoreType.DMA,
        ],
        compiler_params=pltpu.CompilerParams(collective_id=0, has_side_effects=True),
        name="gather_rows",
    )(own)


def expert_kernel(
    n_sp,
    n_tp,
    cap,
    batch,
    rows_ref,
    gate_ref,
    up_ref,
    down_ref,
    out_ref,
    in_ref,
    part_ref,
    half_ref,
    sum_ref,
    in_send,
    in_recv,
    twin_send,
    twin_recv,
    back_send,
    back_recv,
    local_sem,
):
    sp, tp = lax.axis_index("sp"), lax.axis_index("tp")
    steps = far_first(n_sp) + [0]
    twins = [(sp, (tp + hop) % n_tp) for hop in range(1, n_tp)]
    targets = [((sp + step) % n_sp, tp) for step in steps]
    origins = [((sp + n_sp - step) % n_sp, tp) for step in steps]
    greet(targets[:-1] + twins)
    copies = []

    def span(index):
        return pl.ds(pl.multiple_of(index * cap, cap), cap)

    keep_in = pltpu.make_async_copy(
        rows_ref.at[span(sp)], in_ref.at[span((n_sp - 1) * n_tp + tp)], local_sem.at[0]
    )
    keep_in.start()
    for place in range(n_sp - 1):
        copies.append(
            send(
                rows_ref.at[span(targets[place][0])],
                in_ref.at[span(place * n_tp + tp)],
                in_send.at[place],
                in_recv.at[place * n_tp + tp],
                targets[place],
            )
        )

    def forward(place):
        block = place * n_tp + tp
        if place < n_sp - 1:
            arrived(in_ref.at[span(block)], in_recv.at[block])
        for hop, twin in enumerate(twins):
            copies.append(
                send(
                    rows_ref.at[span(sp)] if place == n_sp - 1 else in_ref.at[span(block)],
                    in_ref.at[span(block)],
                    in_send.at[n_sp - 1 + hop * n_sp + place],
                    in_recv.at[block],
                    twin,
                )
            )

    def compute(places):
        for place in places:
            for twin in twins:
                block = place * n_tp + twin[1]
                arrived(in_ref.at[span(block)], in_recv.at[block])
        if places[-1] == n_sp - 1:
            keep_in.wait()
        whole = slice(places[0] * n_tp * cap, (places[-1] + 1) * n_tp * cap)
        rows = in_ref[whole, :]
        gate = jnp.dot(rows, gate_ref[...], preferred_element_type=jnp.float32)
        up = jnp.dot(rows, up_ref[...], preferred_element_type=jnp.float32)
        activated = (gate / (1.0 + jnp.exp(-gate)) * up).astype(jnp.bfloat16)
        part_ref[whole, :] = jnp.dot(
            activated, down_ref[...], preferred_element_type=jnp.float32
        ).astype(jnp.bfloat16)
        for place in places:
            for hop, twin in enumerate(twins):
                slot = hop * n_sp + place
                copies.append(
                    send(
                        part_ref.at[span(place * n_tp + twin[1])],
                        half_ref.at[span(slot)],
                        twin_send.at[slot],
                        twin_recv.at[slot],
                        twin,
                    )
                )

    def finish(places):
        for place in places:
            value = part_ref[span(place * n_tp + tp), :].astype(jnp.float32)
            for hop in range(n_tp - 1):
                slot = hop * n_sp + place
                arrived(half_ref.at[span(slot)], twin_recv.at[slot])
                value = value + half_ref[span(slot), :].astype(jnp.float32)
            if place == n_sp - 1:
                out_ref[span(sp), :] = value.astype(out_ref.dtype)
            else:
                sum_ref[span(place), :] = value.astype(sum_ref.dtype)
                copies.append(
                    send(
                        sum_ref.at[span(place)],
                        out_ref.at[span(sp)],
                        back_send.at[place],
                        back_recv.at[sp],
                        origins[place],
                    )
                )

    batches = [list(range(n_sp))[first : first + batch] for first in range(0, n_sp, batch)]
    for place in batches[0]:
        forward(place)
    for number, places in enumerate(batches):
        compute(places)
        if number > 0:
            finish(batches[number - 1])
        if number + 1 < len(batches):
            for place in batches[number + 1]:
                forward(place)
    finish(batches[-1])
    for target in targets[:-1]:
        arrived(out_ref.at[span(target[0])], back_recv.at[target[0]])
    for copy in copies:
        copy.wait_send()


def expert_rows(rows, gate, up, down, n_sp, n_tp):
    cap = rows.shape[0] // n_sp
    width = rows.shape[1]
    dma = pltpu.SemaphoreType.DMA
    return pl.pallas_call(
        functools.partial(expert_kernel, n_sp, n_tp, cap, math.gcd(n_sp, 256 // (n_tp * cap))),
        out_shape=jax.ShapeDtypeStruct(rows.shape, rows.dtype),
        in_specs=[VMEM] * 4,
        out_specs=VMEM,
        scratch_shapes=[
            pltpu.VMEM((n_sp * n_tp * cap, width), rows.dtype),
            pltpu.VMEM((n_sp * n_tp * cap, width), rows.dtype),
            pltpu.VMEM((n_sp * (n_tp - 1) * cap, width), rows.dtype),
            pltpu.VMEM(rows.shape, rows.dtype),
            dma((n_sp - 1 + n_sp * (n_tp - 1),)),
            dma((n_sp * n_tp,)),
            dma((n_sp * (n_tp - 1),)),
            dma((n_sp * (n_tp - 1),)),
            dma((n_sp - 1,)),
            dma((n_sp,)),
            dma((1,)),
        ],
        compiler_params=pltpu.CompilerParams(collective_id=1, has_side_effects=True),
        name="expert_rows",
    )(rows, gate, up, down)


NT = (((1,), (1,)), ((), ()))


def attention_kernel(
    key_block, latent_width, heads, base_ref, query_ref, kv_ref, key_up_ref, value_up_ref, out_ref, max_ref, sum_ref, acc_ref
):
    first = base_ref[0]
    queries = query_ref.shape[2]
    scale = (QK_NOPE + QK_ROPE) ** (-0.5) * math.log2(math.e)
    max_ref[...] = jnp.full_like(max_ref, NEG_LARGE)
    sum_ref[...] = jnp.zeros_like(sum_ref)
    acc_ref[...] = jnp.zeros_like(acc_ref)

    def block(start, masked):
        start = pl.multiple_of(start, key_block)
        rows = kv_ref[pl.ds(start, key_block), :]
        latent = rows[:, :latent_width]
        rot = rows[:, latent_width:]
        keys = jnp.dot(latent, key_up_ref[...], preferred_element_type=jnp.float32).astype(
            jnp.bfloat16
        )
        values = lax.dot_general(
            value_up_ref[...], latent, NT, preferred_element_type=jnp.float32
        ).astype(jnp.bfloat16)
        if masked:
            key_segment = (
                start + lax.broadcasted_iota(jnp.int32, (key_block, queries), 0)
            ) // SEGMENT
            query_segment = (
                first + lax.broadcasted_iota(jnp.int32, (key_block, queries), 1)
            ) // SEGMENT
            allowed = key_segment <= query_segment
        for head in range(heads):
            wide = jnp.concatenate([keys[:, head * QK_NOPE : (head + 1) * QK_NOPE], rot], axis=1)
            scores = jnp.dot(wide, query_ref[head], preferred_element_type=jnp.float32)
            if masked:
                scores = jnp.where(allowed, scores, NEG_LARGE)
            old_max = max_ref[head]
            new_max = jnp.maximum(old_max, jnp.max(scores, axis=0, keepdims=True))
            weights = jnp.exp2((scores - new_max) * scale)
            shrink = jnp.exp2((old_max - new_max) * scale)
            max_ref[head] = new_max
            sum_ref[head] = sum_ref[head] * shrink + jnp.sum(weights, axis=0, keepdims=True)
            acc_ref[head] = acc_ref[head] * shrink + jnp.dot(
                values[head * V_DIM : (head + 1) * V_DIM],
                weights.astype(jnp.bfloat16),
                preferred_element_type=jnp.float32,
            )

    whole = first // key_block

    def body(step, carry):
        block(step * key_block, False)
        return carry

    lax.fori_loop(0, whole, body, 0)
    block(whole * key_block, True)
    for head in range(heads):
        out_ref[:, head * V_DIM : (head + 1) * V_DIM] = (
            (acc_ref[head] / sum_ref[head]).T.astype(out_ref.dtype)
        )


def attention(base, query, kv, key_up, value_up_t, key_block, latent_width):
    heads, unused, queries = query.shape
    return pl.pallas_call(
        functools.partial(attention_kernel, key_block, latent_width, heads),
        out_shape=jax.ShapeDtypeStruct((queries, heads * V_DIM), jnp.bfloat16),
        in_specs=[pl.BlockSpec(memory_space=pltpu.SMEM), VMEM, VMEM, VMEM, VMEM],
        out_specs=VMEM,
        scratch_shapes=[
            pltpu.VMEM((heads, 1, queries), jnp.float32),
            pltpu.VMEM((heads, 1, queries), jnp.float32),
            pltpu.VMEM((heads, V_DIM, queries), jnp.float32),
        ],
        name="attention",
    )(base, query, kv, key_up, value_up_t)


def local(
    residual,
    query_nope,
    query_rope,
    latent,
    key_rope,
    key_up,
    value_up,
    out_proj,
    norm_gain,
    routes,
    route_weight,
    w_gate,
    w_up,
    w_down,
):
    tp_count = lax.axis_size("tp")
    sp_count = lax.axis_size("sp")
    tp_index = lax.axis_index("tp")
    sp_index = lax.axis_index("sp")
    row_count = residual.shape[0]
    tok_dev = query_nope.shape[0]
    heads_here = query_nope.shape[1] // QK_NOPE
    query_first = sp_index * tok_dev
    query_pos = query_first + jnp.arange(tok_dev, dtype=jnp.int32)
    query_rot = rotary(
        query_rope.astype(jnp.float32).reshape(tok_dev, heads_here, QK_ROPE), query_pos
    ).astype(jnp.bfloat16)
    query_heads = query_nope.reshape(tok_dev, heads_here, QK_NOPE)
    key_pos = query_first + tp_index * row_count + jnp.arange(row_count, dtype=jnp.int32)
    key_rot = rotary(key_rope.astype(jnp.float32), key_pos).astype(jnp.bfloat16)
    width_pad = -(-QK_ROPE // 128) * 128 - QK_ROPE
    packed = jnp.concatenate(
        [latent, key_rot, jnp.zeros((row_count, width_pad), jnp.bfloat16)], axis=1
    )
    gathered = gather_rows(packed, sp_count, tp_count)
    kv_rows = gathered.reshape(sp_count * tok_dev, packed.shape[1])
    query = jnp.concatenate(
        [query_heads, query_rot, jnp.zeros((tok_dev, heads_here, width_pad), jnp.bfloat16)], axis=2
    ).transpose(1, 2, 0)
    key_block = tok_dev * math.gcd(sp_count, 2)
    attn_out = attention(
        query_first.astype(jnp.int32).reshape(1),
        query,
        kv_rows,
        key_up,
        value_up.T,
        key_block,
        latent.shape[1],
    )
    all_heads = lax.all_to_all(attn_out, "tp", split_axis=0, concat_axis=1, tiled=True)
    projected = jnp.dot(all_heads, out_proj, preferred_element_type=jnp.float32)
    hidden_wide = residual.astype(jnp.float32) + projected
    hidden = hidden_wide.astype(jnp.bfloat16)
    hidden_wide = hidden.astype(jnp.float32)
    normed = hidden_wide * lax.rsqrt(
        jnp.mean(hidden_wide * hidden_wide, axis=-1, keepdims=True) + EPSILON
    )
    normed = (normed * norm_gain[None, :]).astype(jnp.bfloat16)
    expert_count = lax.axis_size("sp")
    capacity = max(2, 2 * (row_count * tp_count) // expert_count)
    capacity = -(-capacity // 16) * 16
    top_count = routes.shape[1]
    width = normed.shape[1]
    flat_expert = routes.reshape(-1)
    onehot = (flat_expert[:, None] == jnp.arange(expert_count, dtype=jnp.int32)[None, :]).astype(
        jnp.int32
    )
    slot_rank = jnp.sum(jnp.cumsum(onehot, axis=0) * onehot, axis=1) - 1
    slot_index = flat_expert * capacity + slot_rank
    slots = slot_index.reshape(row_count, top_count)
    slot_count = expert_count * capacity
    numbers = jnp.arange(slot_count, dtype=jnp.int32)
    chosen = slots[:, :, None] == numbers[None, None, :]
    place = jnp.any(chosen, axis=1).astype(jnp.bfloat16)
    outgoing = lax.dot_general(
        place, normed, (((0,), (0,)), ((), ())), preferred_element_type=jnp.float32
    ).astype(jnp.bfloat16)
    shares = jnp.sum(jnp.where(chosen, route_weight[:, :, None], 0.0), axis=1)
    share_high = lax.reduce_precision(shares, 8, 7)
    share_low = shares - share_high
    back_rows = expert_rows(outgoing, w_gate[0], w_up[0], w_down[0], sp_count, tp_count)
    combined = jnp.dot(
        share_high.astype(jnp.bfloat16), back_rows, preferred_element_type=jnp.float32
    ) + jnp.dot(share_low.astype(jnp.bfloat16), back_rows, preferred_element_type=jnp.float32)
    return (hidden_wide + combined).astype(jnp.bfloat16)


def solution(mesh):
    return jax.shard_map(
        local,
        mesh=mesh,
        in_specs=(
            P(("sp", "tp"), None),
            P("sp", "tp"),
            P("sp", "tp"),
            P(("sp", "tp"), None),
            P(("sp", "tp"), None),
            P(None, "tp"),
            P(None, "tp"),
            P(),
            P(),
            P(("sp", "tp"), None),
            P(("sp", "tp"), None),
            P("sp", None, "tp"),
            P("sp", None, "tp"),
            P("sp", "tp", None),
        ),
        out_specs=P(("sp", "tp"), None),
        check_vma=False,
    )
```

```python
import functools
import math

import jax
import jax.numpy as jnp
from jax import lax
from jax.experimental import pallas as pl
from jax.experimental.pallas import tpu as pltpu
from jax.sharding import PartitionSpec as P

QK_NOPE = 128
QK_ROPE = 64
V_DIM = 128
SEGMENT = 64


EPSILON = 1e-06
ROPE_BASE = 10000.0
NEG_LARGE = -1e30


def rotary(values, positions):
    half_width = values.shape[-1] // 2
    inverse = ROPE_BASE ** (-2.0 * jnp.arange(half_width, dtype=jnp.float32) / values.shape[-1])
    angles = positions.astype(jnp.float32)[:, None] * inverse[None, :]
    cosine = jnp.cos(angles)
    sine_part = jnp.sin(angles)
    if values.ndim == 3:
        cosine = cosine[:, None, :]
        sine_part = sine_part[:, None, :]
    first_half = values[..., :half_width]
    second = values[..., half_width:]
    return jnp.concatenate(
        [first_half * cosine - second * sine_part, second * cosine + first_half * sine_part],
        axis=-1,
    )


MESH = pl.DeviceIdType.MESH
VMEM = pl.BlockSpec(memory_space=pltpu.VMEM)


def greet(peers):
    barrier = pltpu.get_barrier_semaphore()
    for peer in peers:
        pl.semaphore_signal(barrier, inc=1, device_id=peer, device_id_type=MESH)
    pl.semaphore_wait(barrier, len(peers))


def far_first(count):
    return sorted(range(1, count), key=lambda step: abs(2 * step - count))


def send(source, target, send_sem, recv_sem, peer):
    copy = pltpu.make_async_remote_copy(
        src_ref=source,
        dst_ref=target,
        send_sem=send_sem,
        recv_sem=recv_sem,
        device_id=peer,
        device_id_type=MESH,
    )
    copy.start()
    return copy


def arrived(block, semaphore):
    pltpu.make_async_copy(block, block, semaphore).wait()


def gather_kernel(n_sp, n_tp, inner, own_ref, out_ref, send_sem, recv_sem, local_sem):
    sp, tp = lax.axis_index("sp"), lax.axis_index("tp")
    outer = n_sp // inner
    group, member = sp // inner, sp % inner

    def column(step):
        return ((group + step) % outer) * inner + member

    def mate(step):
        return group * inner + (member + step) % inner

    others = [(column(step), tp) for step in far_first(outer)]
    mates = [(mate(step), tp) for step in range(1, inner)]
    twins = [(sp, (tp + step) % n_tp) for step in range(1, n_tp)]
    greet(others + mates + twins)
    copies = []

    def push(source, block, peers):
        for peer in peers:
            copies.append(
                send(
                    source, out_ref.at[block], send_sem.at[len(copies)], recv_sem.at[block], peer
                )
            )

    mine = sp * n_tp + tp
    keep = pltpu.make_async_copy(own_ref, out_ref.at[mine], local_sem)
    keep.start()
    push(own_ref, mine, others + mates + twins)
    for step in sorted(range(1, outer), key=lambda step: min(step, outer - step)):
        block = column(step) * n_tp + tp
        arrived(out_ref.at[block], recv_sem.at[block])
        push(out_ref.at[block], block, mates + twins)
    for step in range(outer):
        for hop in range(1, inner):
            source = ((group + step) % outer) * inner + (member + hop) % inner
            block = source * n_tp + tp
            arrived(out_ref.at[block], recv_sem.at[block])
            push(out_ref.at[block], block, twins)
    for twin in twins:
        for source in range(n_sp):
            block = source * n_tp + twin[1]
            arrived(out_ref.at[block], recv_sem.at[block])
    keep.wait()
    for copy in copies:
        copy.wait_send()


def gather_rows(own, n_sp, n_tp):
    inner = math.gcd(n_sp, 4)
    outer = n_sp // inner
    sends = (outer - 1) + outer * (inner - 1) + n_sp * (n_tp - 1)
    return pl.pallas_call(
        functools.partial(gather_kernel, n_sp, n_tp, inner),
        out_shape=jax.ShapeDtypeStruct((n_sp * n_tp,) + own.shape, own.dtype),
        in_specs=[VMEM],
        out_specs=VMEM,
        scratch_shapes=[
            pltpu.SemaphoreType.DMA((sends,)),
            pltpu.SemaphoreType.DMA((n_sp * n_tp,)),
            pltpu.SemaphoreType.DMA,
        ],
        compiler_params=pltpu.CompilerParams(collective_id=0, has_side_effects=True),
        name="gather_rows",
    )(own)


def expert_kernel(
    n_sp,
    n_tp,
    cap,
    batch,
    rows_ref,
    gate_ref,
    up_ref,
    down_ref,
    out_ref,
    in_ref,
    part_ref,
    half_ref,
    sum_ref,
    in_send,
    in_recv,
    twin_send,
    twin_recv,
    back_send,
    back_recv,
    local_sem,
):
    sp, tp = lax.axis_index("sp"), lax.axis_index("tp")
    steps = far_first(n_sp) + [0]
    twins = [(sp, (tp + hop) % n_tp) for hop in range(1, n_tp)]
    targets = [((sp + step) % n_sp, tp) for step in steps]
    origins = [((sp + n_sp - step) % n_sp, tp) for step in steps]
    greet(targets[:-1] + twins)
    copies = []

    def span(index):
        return pl.ds(pl.multiple_of(index * cap, cap), cap)

    keep_in = pltpu.make_async_copy(
        rows_ref.at[span(sp)], in_ref.at[span((n_sp - 1) * n_tp + tp)], local_sem.at[0]
    )
    keep_in.start()
    for place in range(n_sp - 1):
        copies.append(
            send(
                rows_ref.at[span(targets[place][0])],
                in_ref.at[span(place * n_tp + tp)],
                in_send.at[place],
                in_recv.at[place * n_tp + tp],
                targets[place],
            )
        )

    def forward(place):
        block = place * n_tp + tp
        if place < n_sp - 1:
            arrived(in_ref.at[span(block)], in_recv.at[block])
        for hop, twin in enumerate(twins):
            copies.append(
                send(
                    rows_ref.at[span(sp)] if place == n_sp - 1 else in_ref.at[span(block)],
                    in_ref.at[span(block)],
                    in_send.at[n_sp - 1 + hop * n_sp + place],
                    in_recv.at[block],
                    twin,
                )
            )

    def compute(places):
        for place in places:
            for twin in twins:
                block = place * n_tp + twin[1]
                arrived(in_ref.at[span(block)], in_recv.at[block])
        if places[-1] == n_sp - 1:
            keep_in.wait()
        whole = slice(places[0] * n_tp * cap, (places[-1] + 1) * n_tp * cap)
        rows = in_ref[whole, :]
        gate = jnp.dot(rows, gate_ref[...], preferred_element_type=jnp.float32)
        up = jnp.dot(rows, up_ref[...], preferred_element_type=jnp.float32)
        activated = (gate / (1.0 + jnp.exp(-gate)) * up).astype(jnp.bfloat16)
        part_ref[whole, :] = jnp.dot(
            activated, down_ref[...], preferred_element_type=jnp.float32
        ).astype(jnp.bfloat16)
        for place in places:
            for hop, twin in enumerate(twins):
                slot = hop * n_sp + place
                copies.append(
                    send(
                        part_ref.at[span(place * n_tp + twin[1])],
                        half_ref.at[span(slot)],
                        twin_send.at[slot],
                        twin_recv.at[slot],
                        twin,
                    )
                )

    def finish(places):
        for place in places:
            value = part_ref[span(place * n_tp + tp), :].astype(jnp.float32)
            for hop in range(n_tp - 1):
                slot = hop * n_sp + place
                arrived(half_ref.at[span(slot)], twin_recv.at[slot])
                value = value + half_ref[span(slot), :].astype(jnp.float32)
            if place == n_sp - 1:
                out_ref[span(sp), :] = value.astype(out_ref.dtype)
            else:
                sum_ref[span(place), :] = value.astype(sum_ref.dtype)
                copies.append(
                    send(
                        sum_ref.at[span(place)],
                        out_ref.at[span(sp)],
                        back_send.at[place],
                        back_recv.at[sp],
                        origins[place],
                    )
                )

    batches = [list(range(n_sp))[first : first + batch] for first in range(0, n_sp, batch)]
    for place in batches[0]:
        forward(place)
    for number, places in enumerate(batches):
        compute(places)
        if number > 0:
            finish(batches[number - 1])
        if number + 1 < len(batches):
            for place in batches[number + 1]:
                forward(place)
    finish(batches[-1])
    for target in targets[:-1]:
        arrived(out_ref.at[span(target[0])], back_recv.at[target[0]])
    for copy in copies:
        copy.wait_send()


def expert_rows(rows, gate, up, down, n_sp, n_tp):
    cap = rows.shape[0] // n_sp
    width = rows.shape[1]
    dma = pltpu.SemaphoreType.DMA
    return pl.pallas_call(
        functools.partial(expert_kernel, n_sp, n_tp, cap, math.gcd(n_sp, 256 // (n_tp * cap))),
        out_shape=jax.ShapeDtypeStruct(rows.shape, rows.dtype),
        in_specs=[VMEM] * 4,
        out_specs=VMEM,
        scratch_shapes=[
            pltpu.VMEM((n_sp * n_tp * cap, width), rows.dtype),
            pltpu.VMEM((n_sp * n_tp * cap, width), rows.dtype),
            pltpu.VMEM((n_sp * (n_tp - 1) * cap, width), rows.dtype),
            pltpu.VMEM(rows.shape, rows.dtype),
            dma((n_sp - 1 + n_sp * (n_tp - 1),)),
            dma((n_sp * n_tp,)),
            dma((n_sp * (n_tp - 1),)),
            dma((n_sp * (n_tp - 1),)),
            dma((n_sp - 1,)),
            dma((n_sp,)),
            dma((1,)),
        ],
        compiler_params=pltpu.CompilerParams(collective_id=1, has_side_effects=True),
        name="expert_rows",
    )(rows, gate, up, down)


def heads_kernel(n_tp, own_ref, out_ref, send_sem, recv_sem, local_sem):
    sp, tp = lax.axis_index("sp"), lax.axis_index("tp")
    twins = [(sp, (tp + hop) % n_tp) for hop in range(1, n_tp)]
    greet(twins)
    rows = out_ref.shape[1]

    def part(core):
        return own_ref.at[pl.ds(pl.multiple_of(core * rows, rows), rows)]

    copies = [
        send(part(twin[1]), out_ref.at[tp], send_sem.at[hop], recv_sem.at[tp], twin)
        for hop, twin in enumerate(twins)
    ]
    keep = pltpu.make_async_copy(part(tp), out_ref.at[tp], local_sem)
    keep.start()
    for twin in twins:
        arrived(out_ref.at[twin[1]], recv_sem.at[twin[1]])
    keep.wait()
    for copy in copies:
        copy.wait_send()


def swap_heads(own, n_tp):
    return pl.pallas_call(
        functools.partial(heads_kernel, n_tp),
        out_shape=jax.ShapeDtypeStruct((n_tp, own.shape[0] // n_tp, own.shape[1]), own.dtype),
        in_specs=[VMEM],
        out_specs=VMEM,
        scratch_shapes=[
            pltpu.SemaphoreType.DMA((n_tp - 1,)),
            pltpu.SemaphoreType.DMA((n_tp,)),
            pltpu.SemaphoreType.DMA,
        ],
        compiler_params=pltpu.CompilerParams(collective_id=2, has_side_effects=True),
        name="swap_heads",
    )(own)


NT = (((1,), (1,)), ((), ()))


def attention_kernel(
    key_block, latent_width, heads, base_ref, query_ref, kv_ref, key_up_ref, value_up_ref, out_ref, max_ref, sum_ref, acc_ref
):
    first = base_ref[0]
    queries = query_ref.shape[2]
    scale = (QK_NOPE + QK_ROPE) ** (-0.5) * math.log2(math.e)
    max_ref[...] = jnp.full_like(max_ref, NEG_LARGE)
    sum_ref[...] = jnp.zeros_like(sum_ref)
    acc_ref[...] = jnp.zeros_like(acc_ref)

    def block(start, masked):
        start = pl.multiple_of(start, key_block)
        rows = kv_ref[pl.ds(start, key_block), :]
        latent = rows[:, :latent_width]
        rot = rows[:, latent_width:]
        keys = jnp.dot(latent, key_up_ref[...], preferred_element_type=jnp.float32).astype(
            jnp.bfloat16
        )
        values = lax.dot_general(
            value_up_ref[...], latent, NT, preferred_element_type=jnp.float32
        ).astype(jnp.bfloat16)
        if masked:
            key_segment = (
                start + lax.broadcasted_iota(jnp.int32, (key_block, queries), 0)
            ) // SEGMENT
            query_segment = (
                first + lax.broadcasted_iota(jnp.int32, (key_block, queries), 1)
            ) // SEGMENT
            allowed = key_segment <= query_segment
        for head in range(heads):
            wide = jnp.concatenate([keys[:, head * QK_NOPE : (head + 1) * QK_NOPE], rot], axis=1)
            scores = jnp.dot(wide, query_ref[head], preferred_element_type=jnp.float32)
            if masked:
                scores = jnp.where(allowed, scores, NEG_LARGE)
            old_max = max_ref[head]
            new_max = jnp.maximum(old_max, jnp.max(scores, axis=0, keepdims=True))
            weights = jnp.exp2((scores - new_max) * scale)
            shrink = jnp.exp2((old_max - new_max) * scale)
            max_ref[head] = new_max
            sum_ref[head] = sum_ref[head] * shrink + jnp.sum(weights, axis=0, keepdims=True)
            acc_ref[head] = acc_ref[head] * shrink + jnp.dot(
                values[head * V_DIM : (head + 1) * V_DIM],
                weights.astype(jnp.bfloat16),
                preferred_element_type=jnp.float32,
            )

    whole = first // key_block

    def body(step, carry):
        block(step * key_block, False)
        return carry

    lax.fori_loop(0, whole, body, 0)
    block(whole * key_block, True)
    for head in range(heads):
        out_ref[:, head * V_DIM : (head + 1) * V_DIM] = (
            (acc_ref[head] / sum_ref[head]).T.astype(out_ref.dtype)
        )


def attention(base, query, kv, key_up, value_up_t, key_block, latent_width):
    heads, unused, queries = query.shape
    return pl.pallas_call(
        functools.partial(attention_kernel, key_block, latent_width, heads),
        out_shape=jax.ShapeDtypeStruct((queries, heads * V_DIM), jnp.bfloat16),
        in_specs=[pl.BlockSpec(memory_space=pltpu.SMEM), VMEM, VMEM, VMEM, VMEM],
        out_specs=VMEM,
        scratch_shapes=[
            pltpu.VMEM((heads, 1, queries), jnp.float32),
            pltpu.VMEM((heads, 1, queries), jnp.float32),
            pltpu.VMEM((heads, V_DIM, queries), jnp.float32),
        ],
        name="attention",
    )(base, query, kv, key_up, value_up_t)


def local(
    residual,
    query_nope,
    query_rope,
    latent,
    key_rope,
    key_up,
    value_up,
    out_proj,
    norm_gain,
    routes,
    route_weight,
    w_gate,
    w_up,
    w_down,
):
    tp_count = lax.axis_size("tp")
    sp_count = lax.axis_size("sp")
    tp_index = lax.axis_index("tp")
    sp_index = lax.axis_index("sp")
    row_count = residual.shape[0]
    tok_dev = query_nope.shape[0]
    heads_here = query_nope.shape[1] // QK_NOPE
    query_first = sp_index * tok_dev
    query_pos = query_first + jnp.arange(tok_dev, dtype=jnp.int32)
    query_rot = rotary(
        query_rope.astype(jnp.float32).reshape(tok_dev, heads_here, QK_ROPE), query_pos
    ).astype(jnp.bfloat16)
    query_heads = query_nope.reshape(tok_dev, heads_here, QK_NOPE)
    key_pos = query_first + tp_index * row_count + jnp.arange(row_count, dtype=jnp.int32)
    key_rot = rotary(key_rope.astype(jnp.float32), key_pos).astype(jnp.bfloat16)
    width_pad = -(-QK_ROPE // 128) * 128 - QK_ROPE
    packed = jnp.concatenate(
        [latent, key_rot, jnp.zeros((row_count, width_pad), jnp.bfloat16)], axis=1
    )
    gathered = gather_rows(packed, sp_count, tp_count)
    kv_rows = gathered.reshape(sp_count * tok_dev, packed.shape[1])
    query = jnp.concatenate(
        [query_heads, query_rot, jnp.zeros((tok_dev, heads_here, width_pad), jnp.bfloat16)], axis=2
    ).transpose(1, 2, 0)
    key_block = tok_dev * math.gcd(sp_count, 2)
    attn_out = attention(
        query_first.astype(jnp.int32).reshape(1),
        query,
        kv_rows,
        key_up,
        value_up.T,
        key_block,
        latent.shape[1],
    )
    all_heads = swap_heads(attn_out, tp_count)
    proj_parts = out_proj.reshape(tp_count, attn_out.shape[1], out_proj.shape[1])
    projected = jnp.dot(all_heads[0], proj_parts[0], preferred_element_type=jnp.float32)
    for core in range(1, tp_count):
        projected = projected + jnp.dot(
            all_heads[core], proj_parts[core], preferred_element_type=jnp.float32
        )
    hidden_wide = residual.astype(jnp.float32) + projected
    hidden = hidden_wide.astype(jnp.bfloat16)
    hidden_wide = hidden.astype(jnp.float32)
    normed = hidden_wide * lax.rsqrt(
        jnp.mean(hidden_wide * hidden_wide, axis=-1, keepdims=True) + EPSILON
    )
    normed = (normed * norm_gain[None, :]).astype(jnp.bfloat16)
    expert_count = lax.axis_size("sp")
    capacity = max(2, 2 * (row_count * tp_count) // expert_count)
    capacity = -(-capacity // 16) * 16
    top_count = routes.shape[1]
    width = normed.shape[1]
    flat_expert = routes.reshape(-1)
    onehot = (flat_expert[:, None] == jnp.arange(expert_count, dtype=jnp.int32)[None, :]).astype(
        jnp.int32
    )
    slot_rank = jnp.sum(jnp.cumsum(onehot, axis=0) * onehot, axis=1) - 1
    slot_index = flat_expert * capacity + slot_rank
    slots = slot_index.reshape(row_count, top_count)
    slot_count = expert_count * capacity
    numbers = jnp.arange(slot_count, dtype=jnp.int32)
    chosen = slots[:, :, None] == numbers[None, None, :]
    place = jnp.any(chosen, axis=1).astype(jnp.bfloat16)
    outgoing = lax.dot_general(
        place, normed, (((0,), (0,)), ((), ())), preferred_element_type=jnp.float32
    ).astype(jnp.bfloat16)
    shares = jnp.sum(jnp.where(chosen, route_weight[:, :, None], 0.0), axis=1)
    share_high = lax.reduce_precision(shares, 8, 7)
    share_low = shares - share_high
    back_rows = expert_rows(outgoing, w_gate[0], w_up[0], w_down[0], sp_count, tp_count)
    combined = jnp.dot(
        share_high.astype(jnp.bfloat16), back_rows, preferred_element_type=jnp.float32
    ) + jnp.dot(share_low.astype(jnp.bfloat16), back_rows, preferred_element_type=jnp.float32)
    return (hidden_wide + combined).astype(jnp.bfloat16)


def solution(mesh):
    return jax.shard_map(
        local,
        mesh=mesh,
        in_specs=(
            P(("sp", "tp"), None),
            P("sp", "tp"),
            P("sp", "tp"),
            P(("sp", "tp"), None),
            P(("sp", "tp"), None),
            P(None, "tp"),
            P(None, "tp"),
            P(),
            P(),
            P(("sp", "tp"), None),
            P(("sp", "tp"), None),
            P("sp", None, "tp"),
            P("sp", None, "tp"),
            P("sp", "tp", None),
        ),
        out_specs=P(("sp", "tp"), None),
        check_vma=False,
    )
```
